32 devices in a mesh: fs: 8 (over z, y), tp: 4 (over x, core).
Axes of the slice: x: 2, y: 2, z: 4, core: 2. Of those that a mesh axis runs over, the one named last changes fastest.
Arguments:
- x_later: bfloat16 [4096, 2048], P(('fs', 'tp')), may hold values from -6 to 6
- x_earlier: bfloat16 [4096, 2048], P(('fs', 'tp')), may hold values from -6 to 6
- d_hidden: bfloat16 [4096, 6144], P('fs', 'tp'), may hold values from -6 to 6
- gate_weight: bfloat16 [2048, 6144], P('fs', 'tp'), may hold values from -0.125 to 0.125
- up_weight: bfloat16 [2048, 6144], P('fs', 'tp'), may hold values from -0.125 to 0.125
- conv_taps: float32 [3, 6144], P(None, 'tp'), may hold values from -3 to 3
- conv_bias: float32 [6144], P('tp'), may hold values from -3 to 3
- gate_sum: float32 [2048, 6144], P('fs', 'tp'), may hold values from -6 to 6
- up_sum: float32 [2048, 6144], P('fs', 'tp'), may hold values from -6 to 6
- taps_sum: float32 [3, 6144], P(None, 'tp'), may hold values from -6 to 6
- bias_sum: float32 [6144], P('tp'), may hold values from -6 to 6
Outputs:
- hidden: bfloat16 [4096, 6144], P('fs', 'tp')
- d_input: bfloat16 [4096, 2048], P(('fs', 'tp'))
- gate_sum_out: float32 [2048, 6144], P('fs', 'tp')
- up_sum_out: float32 [2048, 6144], P('fs', 'tp')
- taps_sum_out: float32 [3, 6144], P(None, 'tp')
- bias_sum_out: float32 [6144], P('tp')
The draws below stay inside these ranges and needn't reach their ends.
All inputs are finite; a program needn't handle non-finite values.
Results may differ from the reference program's by a relative error of at most 0.018.
Values may be sent and summed in bfloat16 or wider, within the bound.
No kernel may reach another device: no remote copies, remote signals or barrier semaphores. Data moves between devices by JAX's collectives and lax.ppermute only.
A program may use at most 128 MiB of HBM per device.

```python
import jax
import jax.numpy as jnp
from jax import lax

D = 2048
FF = 6144
KW = 3
LEN = 512
TOKENS = 4096
N_FS = 8
N_TP = 4


def spiked(array, key, source, target, blocks, factor):
    owner, partner = [(jnp.arange(array.shape[dim]) // (array.shape[dim] // blocks)).reshape([-1 if axis == dim else 1 for axis in range(array.ndim)]) for dim in (source, target)]
    chosen = jax.random.permutation(key, blocks)[partner]
    strong = (owner == chosen) | (owner == (partner + blocks // 2) % blocks)
    return jnp.where(strong, factor * array, array)


def level_of(key, shape, cuts, low, top_value):
    level = 1.0
    for position, blocks in cuts:
        heights = jax.random.uniform(jax.random.fold_in(jax.random.fold_in(key, 6), position), (blocks,), jnp.float32, low / len(cuts), top_value / len(cuts))
        level = level * jnp.repeat(jnp.exp(heights), shape[position] // blocks).reshape((-1,) + (1,) * (len(shape) - 1 - position))
    return level


def bell_draw(stream_key, shape, deviation, bound, split=(), dtype=jnp.bfloat16):
    result = deviation * jax.random.normal(stream_key, shape, jnp.float32)
    if split:
        result = result * level_of(stream_key, shape, split, -0.22, 0.18)
    return jnp.clip(result, -bound, bound).astype(dtype)


def bell_draw_with(stream_key, shape, spread, most, pieces, heavy, held_as=jnp.bfloat16):
    drawn = spread * jax.random.normal(stream_key, shape, jnp.float32)
    if pieces:
        drawn = drawn * level_of(stream_key, shape, pieces, -0.22, 0.18)
    return jnp.clip(spiked(drawn, jax.random.fold_in(stream_key, 3), *heavy), -most, most).astype(held_as)


def setup_inputs(seed: int = 0) -> dict:
    key_of = jax.random.split(jax.random.key(seed), 12)
    return {
        "x_later": bell_draw(key_of[0], (TOKENS, D), 1.0, 6.0, ((0, 32),)),
        "x_earlier": bell_draw(key_of[1], (TOKENS, D), 1.0, 6.0, ((0, 32),)),
        "d_hidden": bell_draw_with(key_of[2], (TOKENS, FF), 1.0, 6.0, ((0, 8), (1, 4)), (0, 1, 8, 2.0)),
        "gate_weight": bell_draw(key_of[3], (D, FF), D ** -0.5, 0.125, ((0, 8), (1, 4))),
        "up_weight": bell_draw(key_of[4], (D, FF), D ** -0.5, 0.125, ((0, 8), (1, 4))),
        "conv_taps": bell_draw(key_of[5], (KW, FF), 0.6, 3.0, ((1, 4),), jnp.float32),
        "conv_bias": bell_draw(key_of[6], (FF,), 0.5, 3.0, ((0, 4),), jnp.float32),
        "gate_sum": bell_draw(key_of[7], (D, FF), 1.0, 6.0, ((0, 8), (1, 4)), jnp.float32),
        "up_sum": bell_draw(key_of[8], (D, FF), 1.0, 6.0, ((0, 8), (1, 4)), jnp.float32),
        "taps_sum": bell_draw(key_of[9], (KW, FF), 1.0, 6.0, ((1, 4),), jnp.float32),
        "bias_sum": bell_draw(key_of[10], (FF,), 1.0, 6.0, ((0, 4),), jnp.float32),
    }


def forward_parts(rows, gate_weight, up_weight, conv_taps, conv_bias):
    gate_lin = jnp.dot(rows, gate_weight, preferred_element_type=jnp.float32).astype(jnp.bfloat16)
    up_lin = jnp.dot(rows, up_weight, preferred_element_type=jnp.float32).astype(jnp.bfloat16)
    width = gate_lin.shape[1]
    seq_gate = gate_lin.astype(jnp.float32).reshape(N_FS, LEN, width)
    padded = jnp.pad(seq_gate, ((0, 0), (KW - 1, 0), (0, 0)))
    pre = jnp.zeros_like(seq_gate) + conv_bias
    for tap in range(KW):
        pre = pre + padded[:, tap:tap + LEN] * conv_taps[tap]
    return (gate_lin, up_lin, padded, pre)

def reference(x_later, x_earlier, d_hidden, gate_weight, up_weight, conv_taps, conv_bias, gate_sum, up_sum, taps_sum, bias_sum):
    width = gate_weight.shape[1]
    _, up_lin, _, pre = forward_parts(x_later, gate_weight, up_weight, conv_taps, conv_bias)
    act = jax.nn.gelu(pre).reshape(-1, width)
    hidden = (act * up_lin.astype(jnp.float32)).astype(jnp.bfloat16)
    gate_lin, up_lin, padded, pre = forward_parts(x_earlier, gate_weight, up_weight, conv_taps, conv_bias)
    act, pull = jax.vjp(jax.nn.gelu, pre)
    cot = d_hidden.astype(jnp.float32).reshape(N_FS, LEN, width)
    d_up = (cot * act).reshape(-1, width).astype(jnp.bfloat16)
    d_pre = pull(cot * up_lin.astype(jnp.float32).reshape(N_FS, LEN, width))[0]
    tail = jnp.pad(d_pre, ((0, 0), (0, KW - 1), (0, 0)))
    d_gate = jnp.zeros_like(d_pre)
    for tap in range(KW):
        start = KW - 1 - tap
        d_gate = d_gate + tail[:, start:start + LEN] * conv_taps[tap]
    d_gate = d_gate.reshape(-1, width).astype(jnp.bfloat16)
    block = width // N_TP
    d_input = jnp.zeros(x_earlier.shape, jnp.float32)
    for part in range(N_TP):
        lo = part * block
        term = jnp.dot(d_gate[:, lo:lo + block], gate_weight[:, lo:lo + block].T, preferred_element_type=jnp.float32)
        term = term + jnp.dot(d_up[:, lo:lo + block], up_weight[:, lo:lo + block].T, preferred_element_type=jnp.float32)
        d_input = d_input + term.astype(jnp.bfloat16).astype(jnp.float32)
    d_input = d_input.astype(jnp.bfloat16)
    factor = 1.0 / TOKENS ** 0.5
    gate_grad = jnp.dot(x_earlier.T, d_gate, preferred_element_type=jnp.float32)
    up_grad = jnp.dot(x_earlier.T, d_up, preferred_element_type=jnp.float32)
    taps_grad = jnp.stack([lax.optimization_barrier(jnp.sum(d_pre * padded[:, tap:tap + LEN], axis=(0, 1))) for tap in range(KW)], axis=0)
    bias_grad = lax.optimization_barrier(jnp.sum(d_pre, axis=(0, 1)))
    return (hidden, d_input, gate_sum + factor * gate_grad, up_sum + factor * up_grad, taps_sum + factor * taps_grad, bias_sum + factor * bias_grad)
```

```python
import jax
import jax.numpy as jnp
from jax import lax
from jax.experimental import pallas as pl
from jax.experimental.pallas import tpu as pltpu
from jax.sharding import PartitionSpec as P

CHUNKS = 2


def ring_order(size):
    minor = 1
    while minor * minor * 4 <= size and size % (minor * 2) == 0:
        minor *= 2
    major = size // minor
    if minor == 1 or major % 2:
        return list(range(size))
    order = [0]
    for a in range(major):
        row = [a * minor + b for b in range(1, minor)]
        order += row if a % 2 == 0 else row[::-1]
    return order + [a * minor for a in range(major - 1, 0, -1)]


def route_plan(rings):
    size = len(rings)
    blocks = sorted(range(size), key=lambda r: (min(r, size - r), r))
    plan = []
    for r in blocks[1:]:
        if 2 * r == size and size > 2:
            plan.append((r, [1, -1]))
        else:
            plan.append((r, [1, 1] if 2 * r <= size else [-1, -1]))
    return blocks, plan


def shift_pairs(rings, step):
    size = len(rings)
    return [(rings[(i + step) % size], rings[i]) for i in range(size)]


def back(rings, block, step):
    return (block - step) % len(rings)


def collect(own, rings, gates=()):
    blocks, plan = route_plan(rings)
    half_rows = own.shape[0] // 2
    held = {blocks[0]: own}
    joined = None
    for block, steps in plan:
        turn = min(block, len(blocks) - block) - 2
        froms = [held[back(rings, block, step)] for step in steps]
        if 0 <= turn < len(gates):
            froms = list(lax.optimization_barrier((*froms, gates[turn])))[:2]
        if steps[0] == steps[1]:
            held[block] = lax.ppermute(froms[0], "fs", shift_pairs(rings, steps[0]))
        else:
            joined = block
            held[block] = [
                lax.ppermute(
                    froms[half][half * half_rows : (half + 1) * half_rows],
                    "fs",
                    shift_pairs(rings, step),
                )
                for half, step in enumerate(steps)
            ]
    pieces = []
    for block in blocks:
        if block != joined:
            pieces.append(held[block])
        elif half_rows % 128 == 0:
            pieces += held[block]
        else:
            pieces.append(jnp.concatenate(held[block], axis=0))
    return pieces


def scatter_sum(terms, rings, marks):
    blocks, plan = route_plan(rings)
    rows = terms.shape[0] // len(blocks)
    half_rows = rows // 2
    held = {}
    for place, block in enumerate(blocks):
        for half in range(2):
            begin = place * rows + half * half_rows
            held[block, half] = [terms[begin : begin + half_rows]]
    split = {block for block, steps in plan if steps[0] != steps[1]}
    for block, steps in plan:
        if back(rings, block, steps[0]) in split:
            split.add(block)

    def total(parts):
        acc = parts[0].astype(jnp.float32)
        for item in parts[1:]:
            acc = acc + item.astype(jnp.float32)
        return acc

    for block, steps in reversed(plan):
        sends = []
        for half, step in enumerate(steps):
            sends.append(total(held[block, half]).astype(terms.dtype))
        if block in split:
            moved = [
                lax.ppermute(item, "fs", [(t, s) for s, t in shift_pairs(rings, step)])
                for item, step in zip(sends, steps)
            ]
        else:
            whole = jnp.concatenate(sends, axis=0)
            whole = lax.ppermute(whole, "fs", [(t, s) for s, t in shift_pairs(rings, steps[0])])
            moved = [whole[:half_rows], whole[half_rows:]]
        marks.append(moved[0])
        for half, step in enumerate(steps):
            held[back(rings, block, step), half].append(moved[half])
    return jnp.concatenate([total(held[blocks[0], half]) for half in range(2)], axis=0)


def sum_over(values, size):
    if size & (size - 1):
        return lax.psum(values, "fs")
    reach = 1
    while reach < size:
        values = values + lax.ppermute(values, "fs", [(i, i ^ reach) for i in range(size)])
        reach *= 2
    return values


def times(rows, pieces, index, block):
    count, depth = rows.shape
    width = pieces[0].shape[1]
    tile = 256 if width % 256 == 0 else width

    def body(index_ref, rows_ref, *refs):
        out_ref = refs[-1]
        acc, begin = None, 0
        for ref in refs[:-1]:
            first = index_ref[begin // block] * block
            cols = pl.ds(pl.multiple_of(first + begin % block, 128), ref.shape[0])
            if block % 128 or ref.shape[0] % 128:
                cols = pl.ds(first + begin % block, ref.shape[0])
            term = jnp.dot(
                rows_ref[:, cols],
                ref[...],
                preferred_element_type=jnp.float32,
            )
            acc = term if acc is None else acc + term
            begin += ref.shape[0]
        out_ref[...] = acc.astype(out_ref.dtype)

    return pl.pallas_call(
        body,
        grid_spec=pltpu.PrefetchScalarGridSpec(
            num_scalar_prefetch=1,
            grid=(width // tile,),
            in_specs=[pl.BlockSpec((count, depth), lambda j, _: (0, 0))]
            + [pl.BlockSpec((p.shape[0], tile), lambda j, _: (0, j)) for p in pieces],
            out_specs=pl.BlockSpec((count, tile), lambda j, _: (0, j)),
        ),
        out_shape=jax.ShapeDtypeStruct((count, width), jnp.bfloat16),
        cost_estimate=pl.CostEstimate(
            flops=2 * count * depth * width,
            bytes_accessed=2 * (count * depth + depth * width + count * width),
            transcendentals=0,
        ),
        name="times",
    )(index, rows, *pieces)


def weight_terms(rows, both, index, block):
    count, depth = rows.shape
    width = both.shape[1]
    wide = block if block % 128 == 0 else depth

    def body(index_ref, rows_ref, both_ref, out_ref):
        out_ref[...] = lax.dot_general(
            rows_ref[...], both_ref[...], (((0,), (0,)), ((), ())),
            preferred_element_type=jnp.float32,
        ).astype(out_ref.dtype)

    return pl.pallas_call(
        body,
        grid_spec=pltpu.PrefetchScalarGridSpec(
            num_scalar_prefetch=1,
            grid=(depth // wide,),
            in_specs=[
                pl.BlockSpec((count, wide), lambda j, at: (0, at[j])),
                pl.BlockSpec((count, width), lambda j, at: (0, 0)),
            ],
            out_specs=pl.BlockSpec((wide, width), lambda j, at: (j, 0)),
        ),
        out_shape=jax.ShapeDtypeStruct((depth, width), jnp.bfloat16),
        cost_estimate=pl.CostEstimate(
            flops=2 * count * depth * width,
            bytes_accessed=2 * (count * depth + depth * width + count * width),
            transcendentals=0,
        ),
        name="weight_terms",
    )(index, rows, both)


def times_transposed(rows, pieces, base, last, index, block):
    count, width = rows.shape
    depth = sum(p.shape[0] for p in pieces)
    tile = 128 if count % 128 == 0 else count
    has_base = base is not None

    def body(index_ref, rows_ref, *refs):
        out_ref = refs[-1]
        begin = 0
        for ref in refs[: len(pieces)]:
            first = index_ref[begin // block] * block
            cols = pl.ds(pl.multiple_of(first + begin % block, 128), ref.shape[0])
            if block % 128 or ref.shape[0] % 128:
                cols = pl.ds(first + begin % block, ref.shape[0])
            term = lax.dot_general(
                rows_ref[...],
                ref[...],
                (((1,), (1,)), ((), ())),
                preferred_element_type=jnp.float32,
            )
            if has_base:
                term = term + refs[len(pieces)][:, cols]
            out_ref[:, cols] = term.astype(out_ref.dtype)
            begin += ref.shape[0]

    extra = [base] if has_base else []
    return pl.pallas_call(
        body,
        grid_spec=pltpu.PrefetchScalarGridSpec(
            num_scalar_prefetch=1,
            grid=(count // tile,),
            in_specs=[pl.BlockSpec((tile, width), lambda i, _: (i, 0))]
            + [pl.BlockSpec(p.shape, lambda i, _: (0, 0)) for p in pieces]
            + [pl.BlockSpec((tile, depth), lambda i, _: (i, 0)) for _ in extra],
            out_specs=pl.BlockSpec((tile, depth), lambda i, _: (i, 0)),
        ),
        out_shape=jax.ShapeDtypeStruct((count, depth), jnp.bfloat16 if last else jnp.float32),
        cost_estimate=pl.CostEstimate(
            flops=2 * count * depth * width,
            bytes_accessed=2 * (count * width + depth * width + 2 * count * depth),
            transcendentals=0,
        ),
        name="times_transposed",
    )(index, rows, *pieces, *extra)


def conv_front(gate_lin, conv_taps, conv_bias):
    taps = conv_taps.shape[0]
    length = gate_lin.shape[0]
    padded = jnp.pad(gate_lin.astype(jnp.float32), ((taps - 1, 0), (0, 0)))
    pre = jnp.zeros(gate_lin.shape, jnp.float32) + conv_bias
    for tap in range(taps):
        pre = pre + padded[tap : tap + length] * conv_taps[tap]
    return (padded, pre)


def local(
    x_later,
    x_earlier,
    d_hidden,
    gate_weight,
    up_weight,
    conv_taps,
    conv_bias,
    gate_sum,
    up_sum,
    taps_sum,
    bias_sum,
):
    fs = lax.axis_size("fs")
    rings = ring_order(fs)
    blocks, _ = route_plan(rings)
    block_width, width = gate_weight.shape
    me = lax.axis_index("fs")
    at = jnp.array(rings, jnp.int32)
    spot_of = jnp.array([rings.index(i) for i in range(fs)], jnp.int32)
    index = at[(spot_of[me] + jnp.array(blocks, jnp.int32)) % fs]

    rows_earlier = lax.all_gather(x_earlier, "tp", axis=0, tiled=True)
    rows_later = lax.all_gather(x_later, "tp", axis=0, tiled=True)
    seq_rows = rows_later.shape[0]
    taps = conv_taps.shape[0]
    total_tokens = seq_rows * fs
    factor = 1.0 / total_tokens**0.5
    chunks = CHUNKS if width % (CHUNKS * 128) == 0 else 1
    span = width // chunks

    hidden, gate_out, up_out, taps_local, bias_local = [], [], [], [], []
    d_rows, gates, kept = None, (), []
    for chunk in range(chunks):
        cols = slice(chunk * span, (chunk + 1) * span)
        tap_part, bias_part = conv_taps[:, cols], conv_bias[cols]
        own = jnp.concatenate([gate_weight[:, cols], up_weight[:, cols]], axis=1)
        if chunk:
            own, _ = lax.optimization_barrier((own, weights))
        weights = collect(own, rings, gates)
        lin = times(rows_earlier, weights, index, block_width)
        padded, pre = conv_front(lin[:, :span], tap_part, bias_part)
        act, pull = jax.vjp(jax.nn.gelu, pre)
        cot = d_hidden[:, cols].astype(jnp.float32)
        d_up = (cot * act).astype(jnp.bfloat16)
        d_pre = pull(cot * lin[:, span:].astype(jnp.float32))[0]
        tail = jnp.pad(d_pre, ((0, taps - 1), (0, 0)))
        d_gate = jnp.zeros_like(d_pre)
        for tap in range(taps):
            begin = taps - 1 - tap
            d_gate = d_gate + tail[begin : begin + seq_rows] * tap_part[tap]
        both = jnp.concatenate([d_gate.astype(jnp.bfloat16), d_up], axis=1)
        grads = weight_terms(rows_earlier, both, index, block_width)
        gates = (lin, grads)
        kept.append((cols, tap_part, bias_part, weights, both))
        marks = []
        grads = scatter_sum(grads, rings, marks)
        gate_out.append(gate_sum[:, cols] + factor * grads[:, :span])
        up_out.append(up_sum[:, cols] + factor * grads[:, span:])
        taps_local.append(
            jnp.stack([jnp.sum(d_pre * padded[t : t + seq_rows], axis=0) for t in range(taps)])
        )
        bias_local.append(jnp.sum(d_pre, axis=0, keepdims=True))
    *outer, _ = lax.optimization_barrier((*[entry[4] for entry in kept], marks[0]))
    for chunk, (cols, tap_part, bias_part, weights, both) in enumerate(kept):
        d_rows = times_transposed(
            outer[chunk], weights, d_rows, chunk == chunks - 1, index, block_width
        )
    for chunk, (cols, tap_part, bias_part, weights, both) in enumerate(kept):
        mark = marks[min(2 * chunk + 2, len(marks) - 1)]
        rows_later, _ = lax.optimization_barrier((rows_later, mark))
        ahead = times(rows_later, weights, index, block_width)
        _, pre_later = conv_front(ahead[:, :span], tap_part, bias_part)
        hidden.append(
            (jax.nn.gelu(pre_later) * ahead[:, span:].astype(jnp.float32)).astype(jnp.bfloat16)
        )
    d_input = lax.psum_scatter(d_rows, "tp", scatter_dimension=0, tiled=True)
    small = jnp.concatenate(
        [jnp.concatenate(taps_local, axis=1), jnp.concatenate(bias_local, axis=1)], axis=0
    )
    small = sum_over(small, fs)
    return (
        jnp.concatenate(hidden, axis=1),
        d_input,
        jnp.concatenate(gate_out, axis=1),
        jnp.concatenate(up_out, axis=1),
        taps_sum + factor * small[:taps],
        bias_sum + factor * small[taps],
    )


def solution(mesh):
    placed = (
        P(("fs", "tp"), None),
        P(("fs", "tp"), None),
        P("fs", "tp"),
        P("fs", "tp"),
        P("fs", "tp"),
        P(None, "tp"),
        P("tp"),
        P("fs", "tp"),
        P("fs", "tp"),
        P(None, "tp"),
        P("tp"),
    )
    return jax.shard_map(
        local,
        mesh=mesh,
        in_specs=placed,
        out_specs=(
            P("fs", "tp"),
            P(("fs", "tp"), None),
            P("fs", "tp"),
            P("fs", "tp"),
            P(None, "tp"),
            P("tp"),
        ),
        check_vma=False,
    )
```
